32 devices in a mesh: sp: 8 (over z, y), tp: 4 (over x, core).
Axes of the slice: x: 2, y: 2, z: 4, core: 2. Of those that a mesh axis runs over, the one named last changes fastest.
Arguments:
- hidden: bfloat16 [2048, 4096], P('sp'), as said below
- key_weight: bfloat16 [4096, 1024], P(None, 'tp'), as said below
- queries: bfloat16 [2048, 4096], P('sp', 'tp'), as said below
- values: bfloat16 [2048, 1024], P('sp', 'tp'), as said below
- map_out: bfloat16 [2048, 8192], P('sp', 'tp'), as said below
- log_sums: float32 [32, 2048], P('tp', 'sp'), as said below
- out_grad: bfloat16 [2048, 4096], P('sp', 'tp'), may hold values from -6 to 6
- mixing: float32 [16], P('tp'), may hold values from 0.3 to 0.8
- out_gain: float32 [256], replicated, may hold values from 0.1 to 1.9
Outputs:
- grad_query: bfloat16 [2048, 4096], P('sp', 'tp')
- grad_key: bfloat16 [2048, 1024], P('sp', 'tp')
- grad_value: bfloat16 [2048, 1024], P('sp', 'tp')
- grad_weight: float32 [4096, 1024], P('sp', 'tp')
The draws below stay inside these ranges and needn't reach their ends.
Inputs may be any that keep to these rules, and one draw needn't show every extreme that they name: `hidden`: inputs of order one. `key_weight`: entries of order 1 / sqrt(4096) times a constant. `queries`: entries of order one. `values`: entries of order one. `log_sums`: for head h, map m and row i: the logarithm of the sum over keys j <= i of exp(scores[h, m](i, j)), with key_rows formed as in the reference program. `map_out`: for head h and map m: the row's weights exp(scores - log_sums) over keys j <= i times the values of key head g(h), rounded to bfloat16.
All inputs are finite; a program needn't handle non-finite values.
Results may differ from the reference program's by a relative error of at most 0.02.
Values may be sent and summed in bfloat16 or wider, within the bound.
A program may use at most 256 MiB of HBM per device.

```python
import math
import jax
import jax.numpy as jnp
from jax import lax

D = 4096
HEADS = 16
KV_HEADS = 4
HEAD_DIM = 128
V_DIM = 256
TOKENS = 2048


def base_arrays(key):
    key_hidden = jax.random.fold_in(key, 101)
    key_weight = jax.random.fold_in(key, 102)
    key_query = jax.random.fold_in(key, 103)
    key_value = jax.random.fold_in(key, 104)
    hidden = jax.random.normal(key_hidden, (TOKENS, D), jnp.float32)
    queries = jax.random.normal(key_query, (TOKENS, HEADS * 2 * HEAD_DIM), jnp.float32)
    weight = jax.random.normal(key_weight, (D, KV_HEADS * 2 * HEAD_DIM), jnp.float32) * (1.5 / math.sqrt(D))
    values = jax.random.normal(key_value, (TOKENS, KV_HEADS * V_DIM), jnp.float32)
    return (hidden.astype(jnp.bfloat16), weight.astype(jnp.bfloat16), queries.astype(jnp.bfloat16), values.astype(jnp.bfloat16))


def forward_arrays(key):
    hidden, weight, queries, values = base_arrays(key)
    key_rows = jnp.dot(hidden, weight, preferred_element_type=jnp.float32).astype(jnp.bfloat16).astype(jnp.float32)
    per_group = HEADS // KV_HEADS
    block_rows = 128 if TOKENS % 128 == 0 else TOKENS
    n_blocks = TOKENS // block_rows
    query_all = queries.astype(jnp.float32).reshape(n_blocks, block_rows, KV_HEADS, per_group, 2, HEAD_DIM)
    key_all = key_rows.reshape(TOKENS, KV_HEADS, 2, HEAD_DIM)
    value_all = values.astype(jnp.float32).reshape(TOKENS, KV_HEADS, V_DIM)
    positions = jnp.arange(TOKENS, dtype=jnp.int32).reshape(n_blocks, block_rows)
    key_pos = jnp.arange(TOKENS, dtype=jnp.int32)
    sums_list, outs_list = ([], [])
    for head_group in range(KV_HEADS):
        key_g = key_all[:, head_group]
        value_g = value_all[:, head_group]

        def one_block(inputs):
            query_block, query_pos = inputs
            scores = jnp.einsum('bpmd,tmd->pmbt', query_block[:, head_group], key_g) * HEAD_DIM ** (-0.5)
            visible = key_pos[None, :] <= query_pos[:, None]
            scores = jnp.where(visible, scores, -1e+30)
            row_max = jnp.max(scores, axis=-1, keepdims=True)
            log_sum = row_max + jnp.log(jnp.sum(jnp.exp(scores - row_max), axis=-1, keepdims=True))
            probs_map = jnp.exp(scores - log_sum)
            outputs = jnp.einsum('pmbt,tv->bpmv', probs_map, value_g)
            return (log_sum[..., 0], outputs)
        sums_g, outs_g = lax.map(one_block, (query_all, positions))
        sums_list.append(jnp.transpose(sums_g, (1, 2, 0, 3)).reshape(per_group * 2, TOKENS))
        outs_list.append(outs_g.reshape(TOKENS, per_group * 2 * V_DIM))
    return (jnp.concatenate(sums_list, axis=0), jnp.concatenate(outs_list, axis=1).astype(jnp.bfloat16))


def draw_hidden(key, part):
    return base_arrays(key)[0]


def draw_key_weight(key, part):
    return base_arrays(key)[1]


def draw_queries(key, part):
    return base_arrays(key)[2]


def draw_values(key, part):
    return base_arrays(key)[3]


def draw_log_sums(key, part):
    return forward_arrays(key)[0]


def draw_map_out(key, part):
    return forward_arrays(key)[1]


def spiked(entries, stream_key, source, target, blocks, factor):
    def block_of(axis_at):
        return (jnp.arange(entries.shape[axis_at]) // (entries.shape[axis_at] // blocks)).reshape((-1,) + (1,) * (entries.ndim - 1 - axis_at))

    first = jax.random.permutation(stream_key, blocks)[block_of(target)]
    second = (block_of(target) + blocks // 2) % blocks
    return jnp.where((block_of(source) == first) | (block_of(source) == second), factor * entries, entries)


def steps_of(stream_key, shape, cuts, smallest, high):
    def one(dim, blocks):
        heights = jax.random.uniform(jax.random.fold_in(jax.random.fold_in(stream_key, 6), dim), (blocks,), jnp.float32, smallest / len(cuts), high / len(cuts))
        return jnp.repeat(jnp.exp(heights), shape[dim] // blocks).reshape((-1,) + (1,) * (len(shape) - dim - 1))

    level = one(*cuts[0])
    for cut in cuts[1:]:
        level = level * one(*cut)
    return level


def bell_draw_with(own_key, extent, deviation, most, cuts, heavy, held_as=jnp.bfloat16):
    entries = deviation * jax.random.normal(own_key, extent, jnp.float32)
    if cuts:
        entries = entries * steps_of(own_key, extent, cuts, -0.22, 0.18)
    return jnp.clip(spiked(entries, jax.random.fold_in(own_key, 3), *heavy), -most, most).astype(held_as)


def setup_inputs(seed: int = 0) -> dict:
    seeds = jax.random.split(jax.random.key(seed), 10)
    hidden = draw_hidden(jax.random.fold_in(seeds[9], 71), 0)
    key_weight = draw_key_weight(jax.random.fold_in(seeds[9], 71), 0)
    queries = draw_queries(jax.random.fold_in(seeds[9], 71), 0)
    values = draw_values(jax.random.fold_in(seeds[9], 71), 0)
    map_out = draw_map_out(jax.random.fold_in(seeds[9], 71), 0)
    log_sums = draw_log_sums(jax.random.fold_in(seeds[9], 71), 0)
    out_grad = bell_draw_with(seeds[6], (TOKENS, HEADS * V_DIM), 1.0, 6.0, ((0, 8), (1, 4)), (0, 1, 8, 2.0))
    mixing = jnp.clip(0.3 + 0.5 * jax.random.uniform(seeds[7], (HEADS,), jnp.float32) ** steps_of(seeds[7], (HEADS,), ((0, 4),), -0.2, 0.2), 0.3, 0.8)
    out_gain = jnp.clip(1.0 + 0.18 * jax.random.normal(seeds[8], (V_DIM,), jnp.float32), 0.1, 1.9)
    return {"hidden": hidden, "key_weight": key_weight, "queries": queries, "values": values, "map_out": map_out, "log_sums": log_sums, "out_grad": out_grad, "mixing": mixing, "out_gain": out_gain}


OUT_SCALE = 0.8
NORM_EPS = 1e-06

def head_terms(out_grad, map_out, mixing, out_gain):
    rows_here = out_grad.shape[0]
    heads_here = mixing.shape[0]
    v_width = out_gain.shape[0]
    maps_out = map_out.astype(jnp.float32).reshape(rows_here, heads_here, 2, v_width)
    pre_norm = maps_out[:, :, 0] - mixing[None, :, None] * maps_out[:, :, 1]
    inverse = lax.rsqrt(lax.optimization_barrier(jnp.mean(pre_norm * pre_norm, axis=-1, keepdims=True)) + NORM_EPS)
    upstream = out_grad.astype(jnp.float32).reshape(rows_here, heads_here, v_width) * out_gain * OUT_SCALE
    d_out = inverse * (upstream - pre_norm * inverse * inverse * lax.optimization_barrier(jnp.mean(upstream * pre_norm, axis=-1, keepdims=True)))
    row_terms = lax.optimization_barrier(jnp.sum(d_out[:, :, None, :] * maps_out, axis=-1)).reshape(rows_here, heads_here * 2)
    return (d_out.reshape(rows_here, heads_here * v_width).astype(jnp.bfloat16), row_terms)

def round_trip(array):
    return lax.optimization_barrier(array.astype(jnp.bfloat16)).astype(jnp.float32)

def block_grads(query_blk, d_blk, log_blk, term_blk, query_pos, key_all, value_all, key_pos, mix_blk):
    scale = query_blk.shape[-1] ** (-0.5)
    log_part = jnp.transpose(log_blk, (1, 2, 3, 0))[..., None]
    term_part = jnp.transpose(term_blk, (1, 2, 3, 0))[..., None]
    scores = jnp.einsum('rgpmd,kgmd->gpmrk', query_blk, key_all) * scale
    visible = key_pos[None, :] <= query_pos[:, None]
    probs_map = jnp.exp(jnp.where(visible, scores - log_part, -1e+30))
    d_attn = jnp.einsum('rgpv,kgv->gprk', d_blk, value_all)
    mix_cols = mix_blk[:, :, None, None]
    weights_a = round_trip(probs_map[:, :, 0] - mix_cols * probs_map[:, :, 1])
    d_scores = round_trip(jnp.stack([probs_map[:, :, 0] * (d_attn - term_part[:, :, 0]), -mix_cols * probs_map[:, :, 1] * (d_attn - term_part[:, :, 1])], axis=2))
    grad_q = jnp.einsum('gpmrk,kgmd->rgpmd', d_scores, key_all) * scale
    grad_k = jnp.einsum('gpmrk,rgpmd->kgmd', d_scores, query_blk) * scale
    grad_v = jnp.einsum('gprk,rgpv->kgv', weights_a, d_blk)
    return (grad_q, grad_k, grad_v)

def reference(hidden, key_weight, queries, values, map_out, log_sums, out_grad, mixing, out_gain):
    total = queries.shape[0]
    per_group = HEADS // KV_HEADS
    key_rows = jnp.dot(hidden, key_weight, preferred_element_type=jnp.float32).astype(jnp.bfloat16)
    d_rows, row_terms = head_terms(out_grad, map_out, mixing, out_gain)
    query_all = queries.astype(jnp.float32).reshape(total, KV_HEADS, per_group, 2, HEAD_DIM)
    key_all = key_rows.astype(jnp.float32).reshape(total, KV_HEADS, 2, HEAD_DIM)
    value_all = values.astype(jnp.float32).reshape(total, KV_HEADS, V_DIM)
    d_all = d_rows.astype(jnp.float32).reshape(total, KV_HEADS, per_group, V_DIM)
    log_all = log_sums.T.reshape(total, KV_HEADS, per_group, 2)
    term_all = row_terms.reshape(total, KV_HEADS, per_group, 2)
    mix_all = mixing.reshape(KV_HEADS, per_group)
    block_rows = 256 if total % 256 == 0 else total
    n_blocks = total // block_rows
    key_pos = jnp.arange(total, dtype=jnp.int32)
    query_list, key_list, value_list = ([], [], [])
    for head_group in range(KV_HEADS):
        query_g = query_all[:, head_group:head_group + 1]
        d_g = d_all[:, head_group:head_group + 1]
        log_g = log_all[:, head_group:head_group + 1]
        term_g = term_all[:, head_group:head_group + 1]
        key_g = key_all[:, head_group:head_group + 1]
        value_g = value_all[:, head_group:head_group + 1]
        mix_g = mix_all[head_group:head_group + 1]

        def step_fn(carry, index):
            acc_key, acc_value = carry
            start = (index * block_rows).astype(jnp.int32)
            query_pos = start + jnp.arange(block_rows, dtype=jnp.int32)
            grad_q, grad_k, grad_v = block_grads(lax.dynamic_slice_in_dim(query_g, start, block_rows, 0), lax.dynamic_slice_in_dim(d_g, start, block_rows, 0), lax.dynamic_slice_in_dim(log_g, start, block_rows, 0), lax.dynamic_slice_in_dim(term_g, start, block_rows, 0), query_pos, key_g, value_g, key_pos, mix_g)
            return ((acc_key + grad_k, acc_value + grad_v), grad_q)
        init = (jnp.zeros((total, 1, 2, HEAD_DIM), jnp.float32), jnp.zeros((total, 1, V_DIM), jnp.float32))
        (acc_key, acc_value), grads_q = lax.scan(step_fn, init, jnp.arange(n_blocks, dtype=jnp.int32))
        query_list.append(grads_q.reshape(total, per_group * 2 * HEAD_DIM))
        key_list.append(acc_key.reshape(total, 2 * HEAD_DIM))
        value_list.append(acc_value.reshape(total, V_DIM))
    grad_query = jnp.concatenate(query_list, axis=1).astype(jnp.bfloat16)
    grad_key = jnp.concatenate(key_list, axis=1).astype(jnp.bfloat16)
    grad_value = jnp.concatenate(value_list, axis=1).astype(jnp.bfloat16)
    grad_weight = lax.dot_general(hidden, grad_key, (((0,), (0,)), ((), ())), preferred_element_type=jnp.float32)
    return (grad_query, grad_key, grad_value, grad_weight)
```

```python
import functools
import math

import jax
import jax.numpy as jnp
from jax import lax
from jax.experimental import pallas as pl
from jax.experimental.pallas import tpu as pltpu
from jax.sharding import PartitionSpec as P

HEAD_DIM = 128
V_DIM = 256
OUT_SCALE = 0.8
NORM_EPS = 1e-06
LOG2E = math.log2(math.e)
VMEM = pltpu.VMEM


def dot_nn(a, b):
    return lax.dot_general(a, b, (((1,), (0,)), ((), ())), preferred_element_type=jnp.float32)


def dot_nt(a, b):
    return lax.dot_general(a, b, (((1,), (1,)), ((), ())), preferred_element_type=jnp.float32)


def dot_tn(a, b):
    return lax.dot_general(a, b, (((0,), (0,)), ((), ())), preferred_element_type=jnp.float32)


def head_terms(heads, og_ref, mo_ref, mix_ref, gain_ref, d_ref, term_ref):
    gain = gain_ref[...] * OUT_SCALE
    cols = []
    for h in range(heads):
        v_cols = pl.ds(h * V_DIM, V_DIM)
        map_a = mo_ref[:, pl.ds(2 * h * V_DIM, V_DIM)].astype(jnp.float32)
        map_b = mo_ref[:, pl.ds((2 * h + 1) * V_DIM, V_DIM)].astype(jnp.float32)
        pre = map_a - mix_ref[h] * map_b
        inv = lax.rsqrt(jnp.mean(pre * pre, axis=-1, keepdims=True) + NORM_EPS)
        up = og_ref[:, v_cols].astype(jnp.float32) * gain
        d_out = inv * (up - pre * (inv * inv * jnp.mean(up * pre, axis=-1, keepdims=True)))
        d_ref[:, v_cols] = d_out.astype(jnp.bfloat16)
        cols.append(jnp.sum(d_out * map_a, axis=-1, keepdims=True))
        cols.append(jnp.sum(d_out * map_b, axis=-1, keepdims=True))
    rows = cols[0].shape[0]
    lane = lax.broadcasted_iota(jnp.int32, (rows, 128), 1)
    packed = jnp.zeros((rows, 128), jnp.float32)
    for at, col in enumerate(cols):
        packed = jnp.where(lane == at, col, packed)
    term_ref[...] = packed.T[: 2 * heads]


def block_grads(heads, groups, kv, q_ref, d_ref, log_ref, term_ref, mix_ref, gq_ref, masked):
    per_group = heads // groups
    scale = HEAD_DIM ** (-0.5)
    k_cols = groups * 2 * HEAD_DIM
    outs_k, outs_v = [], []
    for g in range(groups):
        keys = [kv[:, (2 * g + m) * HEAD_DIM : (2 * g + m + 1) * HEAD_DIM] for m in range(2)]
        keys_t = [k.T for k in keys]
        vals = kv[:, k_cols + g * V_DIM : k_cols + (g + 1) * V_DIM]
        grad_k = [None, None]
        grad_v = None
        for h in range(g * per_group, (g + 1) * per_group):
            mix = mix_ref[h]
            d_h = d_ref[:, h * V_DIM : (h + 1) * V_DIM]
            d_attn = dot_nt(vals, d_h)
            qs, probs = [], []
            for m in range(2):
                at = 2 * h + m
                q = q_ref[:, at * HEAD_DIM : (at + 1) * HEAD_DIM]
                s = dot_nt(keys[m], q)
                p = jnp.exp2(s * (scale * LOG2E) - log_ref[at : at + 1, :] * LOG2E)
                if masked:
                    k_at = lax.broadcasted_iota(jnp.int32, p.shape, 0)
                    q_at = lax.broadcasted_iota(jnp.int32, p.shape, 1)
                    p = jnp.where(k_at <= q_at, p, 0.0)
                qs.append(q)
                probs.append(p)
            mixed = mix * probs[1]
            w = (probs[0] - mixed).astype(jnp.bfloat16)
            ds = [
                (probs[0] * (d_attn - term_ref[2 * h : 2 * h + 1, :])).astype(jnp.bfloat16),
                (mixed * (term_ref[2 * h + 1 : 2 * h + 2, :] - d_attn)).astype(jnp.bfloat16),
            ]
            for m in range(2):
                at = 2 * h + m
                gq_ref[at * HEAD_DIM : (at + 1) * HEAD_DIM, :] += dot_nn(keys_t[m], ds[m])
                gk = dot_nn(ds[m], qs[m])
                grad_k[m] = gk if grad_k[m] is None else grad_k[m] + gk
            gv = dot_nn(w, d_h)
            grad_v = gv if grad_v is None else grad_v + gv
        outs_k += [gk * scale for gk in grad_k]
        outs_v.append(grad_v)
    return outs_k + outs_v


def store_cols(ref, rows, pieces):
    at = 0
    for piece in pieces:
        ref[rows, at : at + piece.shape[1]] = piece.astype(ref.dtype)
        at += piece.shape[1]


def attend_kernel(
    n, heads, groups,
    kv_ref, q_ref, mo_ref, og_ref, log_ref, gain_ref, mix_ref,
    gq_out, gkv_out,
    d_ref, term_ref, gq_ref,
):
    me = lax.axis_index("sp")
    rows = q_ref.shape[0]
    head_terms(heads, og_ref, mo_ref, mix_ref, gain_ref, d_ref, term_ref)
    gq_ref[...] = jnp.zeros_like(gq_ref)

    def rows_of(j):
        return pl.ds(pl.multiple_of(j * rows, rows), rows)

    def step(j, masked):
        pieces = block_grads(
            heads, groups, kv_ref[rows_of(j), :], q_ref, d_ref, log_ref, term_ref, mix_ref, gq_ref, masked
        )
        store_cols(gkv_out, rows_of(j), pieces)

    step(me, True)

    @pl.loop(0, me)
    def _(j):
        step(j, False)

    @pl.loop(me + 1, n)
    def _(j):
        gkv_out[rows_of(j), :] = jnp.zeros((rows, gkv_out.shape[1]), gkv_out.dtype)

    for at in range(2 * heads):
        cols = slice(at * HEAD_DIM, (at + 1) * HEAD_DIM)
        gq_out[:, cols] = (gq_ref[cols, :] * HEAD_DIM ** (-0.5)).T.astype(gq_out.dtype)


def on_device(n, hidden, key_weight, queries, values, map_out, log_sums, out_grad, mixing, out_gain):
    rows = queries.shape[0]
    heads = mixing.shape[0]
    groups = values.shape[1] // V_DIM
    k_cols = key_weight.shape[1]
    key_rows = jnp.dot(hidden, key_weight, preferred_element_type=jnp.float32).astype(jnp.bfloat16)
    kv = lax.all_gather(jnp.concatenate([key_rows, values], axis=1), "sp", axis=0, tiled=True)
    vm = pl.BlockSpec(memory_space=VMEM)
    grad_query, grad_kv = pl.pallas_call(
        functools.partial(attend_kernel, n, heads, groups),
        out_shape=(
            jax.ShapeDtypeStruct(queries.shape, jnp.bfloat16),
            jax.ShapeDtypeStruct(kv.shape, jnp.bfloat16),
        ),
        in_specs=[vm] * 6 + [pl.BlockSpec(memory_space=pltpu.SMEM)],
        out_specs=(vm, vm),
        scratch_shapes=[
            VMEM((rows, heads * V_DIM), jnp.bfloat16),
            VMEM((2 * heads, rows), jnp.float32),
            VMEM((2 * heads * HEAD_DIM, rows), jnp.float32),
        ],
        compiler_params=pltpu.CompilerParams(vmem_limit_bytes=56 * 2**20),
        cost_estimate=pl.CostEstimate(flops=5 * 10**9, bytes_accessed=10**7, transcendentals=0),
    )(kv, queries, map_out, out_grad, log_sums, out_gain.reshape(1, V_DIM), mixing)
    own = lax.psum_scatter(grad_kv, "sp", scatter_dimension=0, tiled=True)
    grad_key, grad_value = own[:, :k_cols], own[:, k_cols:]
    grad_weight = lax.psum_scatter(
        dot_tn(hidden, grad_key).astype(jnp.bfloat16), "sp", scatter_dimension=0, tiled=True
    ).astype(jnp.float32)
    return grad_query, grad_key, grad_value, grad_weight


def solution(mesh):
    placed = (
        P("sp", None),
        P(None, "tp"),
        P("sp", "tp"),
        P("sp", "tp"),
        P("sp", "tp"),
        P("tp", "sp"),
        P("sp", "tp"),
        P("tp"),
        P(),
    )
    return jax.shard_map(
        functools.partial(on_device, mesh.shape["sp"]),
        mesh=mesh,
        in_specs=placed,
        out_specs=(P("sp", "tp"), P("sp", "tp"), P("sp", "tp"), P("sp", "tp")),
        check_vma=False,
    )
```

```python
import functools
import math

import jax
import jax.numpy as jnp
from jax import lax
from jax.experimental import pallas as pl
from jax.experimental.pallas import tpu as pltpu
from jax.sharding import PartitionSpec as P

HEAD_DIM = 128
V_DIM = 256
OUT_SCALE = 0.8
NORM_EPS = 1e-06
LOG2E = math.log2(math.e)
VMEM = pltpu.VMEM


def dot_nn(a, b):
    return lax.dot_general(a, b, (((1,), (0,)), ((), ())), preferred_element_type=jnp.float32)


def dot_nt(a, b):
    return lax.dot_general(a, b, (((1,), (1,)), ((), ())), preferred_element_type=jnp.float32)


def dot_tn(a, b):
    return lax.dot_general(a, b, (((0,), (0,)), ((), ())), preferred_element_type=jnp.float32)


def head_terms(heads, og_ref, mo_ref, mix_ref, gain_ref, d_ref, term_ref):
    gain = gain_ref[...] * OUT_SCALE
    cols = []
    for h in range(heads):
        v_cols = pl.ds(h * V_DIM, V_DIM)
        map_a = mo_ref[:, pl.ds(2 * h * V_DIM, V_DIM)].astype(jnp.float32)
        map_b = mo_ref[:, pl.ds((2 * h + 1) * V_DIM, V_DIM)].astype(jnp.float32)
        pre = map_a - mix_ref[h] * map_b
        inv = lax.rsqrt(jnp.mean(pre * pre, axis=-1, keepdims=True) + NORM_EPS)
        up = og_ref[:, v_cols].astype(jnp.float32) * gain
        d_out = inv * (up - pre * (inv * inv * jnp.mean(up * pre, axis=-1, keepdims=True)))
        d_ref[:, v_cols] = d_out.astype(jnp.bfloat16)
        cols.append(jnp.sum(d_out * map_a, axis=-1, keepdims=True))
        cols.append(jnp.sum(d_out * map_b, axis=-1, keepdims=True))
    rows = cols[0].shape[0]
    lane = lax.broadcasted_iota(jnp.int32, (rows, 128), 1)
    packed = jnp.zeros((rows, 128), jnp.float32)
    for at, col in enumerate(cols):
        packed = jnp.where(lane == at, col, packed)
    term_ref[...] = packed.T[: 2 * heads]


def block_grads(heads, groups, k_ref, v_ref, q_ref, d_ref, log_ref, term_ref, mix_ref, gq_ref, masked):
    per_group = heads // groups
    scale = HEAD_DIM ** (-0.5)
    outs_k, outs_v = [], []
    for g in range(groups):
        keys = [k_ref[:, (2 * g + m) * HEAD_DIM : (2 * g + m + 1) * HEAD_DIM] for m in range(2)]
        keys_t = [k.T for k in keys]
        vals = v_ref[:, g * V_DIM : (g + 1) * V_DIM]
        grad_k = [None, None]
        grad_v = None
        for h in range(g * per_group, (g + 1) * per_group):
            mix = mix_ref[h]
            d_h = d_ref[:, h * V_DIM : (h + 1) * V_DIM]
            d_attn = dot_nt(vals, d_h)
            qs, probs = [], []
            for m in range(2):
                at = 2 * h + m
                q = q_ref[:, at * HEAD_DIM : (at + 1) * HEAD_DIM]
                s = dot_nt(keys[m], q)
                p = jnp.exp2(s * (scale * LOG2E) - log_ref[at : at + 1, :] * LOG2E)
                if masked:
                    k_at = lax.broadcasted_iota(jnp.int32, p.shape, 0)
                    q_at = lax.broadcasted_iota(jnp.int32, p.shape, 1)
                    p = jnp.where(k_at <= q_at, p, 0.0)
                qs.append(q)
                probs.append(p)
            mixed = mix * probs[1]
            w = (probs[0] - mixed).astype(jnp.bfloat16)
            ds = [
                (probs[0] * (d_attn - term_ref[2 * h : 2 * h + 1, :])).astype(jnp.bfloat16),
                (mixed * (term_ref[2 * h + 1 : 2 * h + 2, :] - d_attn)).astype(jnp.bfloat16),
            ]
            for m in range(2):
                at = 2 * h + m
                gq_ref[at * HEAD_DIM : (at + 1) * HEAD_DIM, :] += dot_nn(keys_t[m], ds[m])
                gk = dot_nn(ds[m], qs[m])
                grad_k[m] = gk if grad_k[m] is None else grad_k[m] + gk
            gv = dot_nn(w, d_h)
            grad_v = gv if grad_v is None else grad_v + gv
        outs_k += [gk * scale for gk in grad_k]
        outs_v.append(grad_v)
    return outs_k, outs_v


def attend_kernel(
    n, heads, groups,
    hidden_ref, weight_ref, values_ref, q_ref, mo_ref, og_ref, log_ref, gain_ref, mix_ref,
    gq_out, gk_out, gv_out,
    d_ref, term_ref, gq_ref, kv_ref, acc_ref, side_out, side_in, down_out, up_in,
    kv_recv, kv_up_sem, kv_side_sem, side_send, side_recv, down_send, up_recv,
):
    me = lax.axis_index("sp")
    outer = n // 2
    o, y = me // 2, me % 2
    has_up = o < outer - 1
    up, down, side = me + 2, me - 2, me + 1 - 2 * y

    def kv_copy(b, part, sems, target, src=None):
        return pltpu.make_async_remote_copy(
            src_ref=kv_ref.at[b, part] if src is None else src,
            dst_ref=kv_ref.at[b, part],
            send_sem=sems.at[b // 2, part],
            recv_sem=kv_recv.at[b, part],
            device_id={"sp": target},
        )

    def side_copy(ob, part):
        return pltpu.make_async_remote_copy(
            src_ref=side_out.at[ob, part],
            dst_ref=side_in.at[ob, part],
            send_sem=side_send.at[ob, part],
            recv_sem=side_recv.at[ob, part],
            device_id={"sp": side},
        )

    def down_copy(ob, part):
        return pltpu.make_async_remote_copy(
            src_ref=down_out.at[ob, part],
            dst_ref=up_in.at[ob, part],
            send_sem=down_send.at[ob, part],
            recv_sem=up_recv.at[ob, part],
            device_id={"sp": down},
        )

    barrier = pltpu.get_barrier_semaphore()
    pl.semaphore_signal(barrier, inc=1, device_id={"sp": side})

    @pl.when(has_up)
    def _():
        pl.semaphore_signal(barrier, inc=1, device_id={"sp": up})

    @pl.when(o > 0)
    def _():
        pl.semaphore_signal(barrier, inc=1, device_id={"sp": down})

    pl.semaphore_wait(barrier, 1 + has_up.astype(jnp.int32) + (o > 0).astype(jnp.int32))

    def start_own(part, src=None):
        @pl.when(has_up)
        def _():
            kv_copy(me, part, kv_up_sem, up, src).start()

        @pl.when(y == 0)
        def _():
            kv_copy(me, part, kv_side_sem, side, src).start()

    start_own(1, values_ref)
    kv_ref[me, 0] = dot_nn(hidden_ref[...], weight_ref[...]).astype(jnp.bfloat16)
    kv_ref[me, 1] = values_ref[...]
    start_own(0)
    head_terms(heads, og_ref, mo_ref, mix_ref, gain_ref, d_ref, term_ref)
    gq_ref[...] = jnp.zeros_like(gq_ref)

    def grads(b, masked):
        return block_grads(
            heads, groups, kv_ref.at[b, 0], kv_ref.at[b, 1], q_ref, d_ref, log_ref, term_ref, mix_ref, gq_ref, masked
        )

    def store(ref, ob, pieces):
        for part in range(2):
            at = 0
            for piece in pieces[part]:
                ref[ob, part, :, at : at + piece.shape[1]] = piece.astype(ref.dtype)
                at += piece.shape[1]

    lag = jnp.where(has_up, o + 2, 2)

    @pl.loop(0, o + lag + 1)
    def _(t):
        @pl.when(t == 0)
        def _():
            store(acc_ref, o, grads(me, True))

        @pl.when((t > 0) & (t <= o))
        def _():
            b = me - 2 * t
            for part in (1, 0):
                kv_copy(b, part, kv_up_sem, up).wait_recv()

                @pl.when(has_up)
                def _():
                    kv_copy(b, part, kv_up_sem, up).start()

                kv_copy(b, part, kv_side_sem, side).start()
            store(acc_ref, o - t, grads(b, False))

        @pl.when((t > 0) & (t <= o + 1) & ((t > 1) | (y == 1)))
        def _():
            ob = o - t + 1
            b = 2 * ob + 1 - y
            for part in (1, 0):
                kv_copy(b, part, kv_side_sem, side).wait_recv()
            store(side_out, ob, grads(b, False))
            for part in range(2):
                side_copy(ob, part).start()

        @pl.when(t >= lag)
        def _():
            ob = o - t + lag
            for part in range(2):
                @pl.when((ob < o) | (y == 0))
                def _():
                    side_copy(ob, part).wait_recv()
                    acc_ref[ob, part] += side_in[ob, part].astype(jnp.float32)

                @pl.when(has_up)
                def _():
                    down_copy(ob, part).wait_recv()
                    acc_ref[ob, part] += up_in[ob, part].astype(jnp.float32)

                @pl.when(ob < o)
                def _():
                    down_out[ob, part] = acc_ref[ob, part].astype(jnp.bfloat16)
                    down_copy(ob, part).start()

        @pl.when(t == o + 1)
        def _():
            for at in range(2 * heads):
                cols = slice(at * HEAD_DIM, (at + 1) * HEAD_DIM)
                gq_out[:, cols] = (gq_ref[cols, :] * HEAD_DIM ** (-0.5)).T.astype(gq_out.dtype)

    gk_out[...] = acc_ref[o, 0].astype(gk_out.dtype)
    gv_out[...] = acc_ref[o, 1].astype(gv_out.dtype)

    @pl.loop(0, o + 1)
    def _(ob):
        for part in range(2):
            @pl.when(has_up)
            def _():
                kv_copy(2 * ob + y, part, kv_up_sem, up).wait_send()

            @pl.when((ob < o) | (y == 0))
            def _():
                kv_copy(2 * ob + y, part, kv_side_sem, side).wait_send()

            @pl.when((ob < o) | (y == 1))
            def _():
                side_copy(ob, part).wait_send()

            @pl.when(ob < o)
            def _():
                down_copy(ob, part).wait_send()


def on_device(n, hidden, key_weight, queries, values, map_out, log_sums, out_grad, mixing, out_gain):
    rows = queries.shape[0]
    heads = mixing.shape[0]
    width = values.shape[1]
    groups = width // V_DIM
    outer = n // 2
    vm = pl.BlockSpec(memory_space=VMEM)
    hops = pltpu.SemaphoreType.DMA((outer, 2))
    grad_query, grad_key, grad_value = pl.pallas_call(
        functools.partial(attend_kernel, n, heads, groups),
        out_shape=(
            jax.ShapeDtypeStruct(queries.shape, jnp.bfloat16),
            jax.ShapeDtypeStruct((rows, width), jnp.bfloat16),
            jax.ShapeDtypeStruct((rows, width), jnp.bfloat16),
        ),
        in_specs=[vm] * 8 + [pl.BlockSpec(memory_space=pltpu.SMEM)],
        out_specs=(vm, vm, vm),
        scratch_shapes=[
            VMEM((rows, heads * V_DIM), jnp.bfloat16),
            VMEM((2 * heads, rows), jnp.float32),
            VMEM((2 * heads * HEAD_DIM, rows), jnp.float32),
            VMEM((n, 2, rows, width), jnp.bfloat16),
            VMEM((outer, 2, rows, width), jnp.float32),
        ]
        + [VMEM((outer, 2, rows, width), jnp.bfloat16)] * 4
        + [pltpu.SemaphoreType.DMA((n, 2))]
        + [hops] * 6,
        compiler_params=pltpu.CompilerParams(
            vmem_limit_bytes=60 * 2**20, collective_id=0, has_side_effects=True
        ),
        cost_estimate=pl.CostEstimate(flops=5 * 10**9, bytes_accessed=10**7, transcendentals=0),
    )(hidden, key_weight, values, queries, map_out, out_grad, log_sums, out_gain.reshape(1, V_DIM), mixing)
    grad_weight = lax.psum_scatter(
        dot_tn(hidden, grad_key).astype(jnp.bfloat16), "sp", scatter_dimension=0, tiled=True
    ).astype(jnp.float32)
    return grad_query, grad_key, grad_value, grad_weight


def solution(mesh):
    placed = (
        P("sp", None),
        P(None, "tp"),
        P("sp", "tp"),
        P("sp", "tp"),
        P("sp", "tp"),
        P("tp", "sp"),
        P("sp", "tp"),
        P("tp"),
        P(),
    )
    return jax.shard_map(
        functools.partial(on_device, mesh.shape["sp"]),
        mesh=mesh,
        in_specs=placed,
        out_specs=(P("sp", "tp"), P("sp", "tp"), P("sp", "tp"), P("sp", "tp")),
        check_vma=False,
    )
```

```python
import functools
import math

import jax
import jax.numpy as jnp
from jax import lax
from jax.experimental import pallas as pl
from jax.experimental.pallas import tpu as pltpu
from jax.sharding import PartitionSpec as P

HEAD_DIM = 128
V_DIM = 256
OUT_SCALE = 0.8
NORM_EPS = 1e-06
LOG2E = math.log2(math.e)
VMEM = pltpu.VMEM


def dot_nn(a, b):
    return lax.dot_general(a, b, (((1,), (0,)), ((), ())), preferred_element_type=jnp.float32)


def dot_nt(a, b):
    return lax.dot_general(a, b, (((1,), (1,)), ((), ())), preferred_element_type=jnp.float32)


def dot_tn(a, b):
    return lax.dot_general(a, b, (((0,), (0,)), ((), ())), preferred_element_type=jnp.float32)


def head_terms(heads, og_ref, mo_ref, mix_ref, gain_ref, d_ref, term_ref):
    gain = gain_ref[...] * OUT_SCALE
    cols = []
    for h in range(heads):
        v_cols = pl.ds(h * V_DIM, V_DIM)
        map_a = mo_ref[:, pl.ds(2 * h * V_DIM, V_DIM)].astype(jnp.float32)
        map_b = mo_ref[:, pl.ds((2 * h + 1) * V_DIM, V_DIM)].astype(jnp.float32)
        pre = map_a - mix_ref[h] * map_b
        inv = lax.rsqrt(jnp.mean(pre * pre, axis=-1, keepdims=True) + NORM_EPS)
        up = og_ref[:, v_cols].astype(jnp.float32) * gain
        d_out = inv * (up - pre * (inv * inv * jnp.mean(up * pre, axis=-1, keepdims=True)))
        d_ref[:, v_cols] = d_out.astype(jnp.bfloat16)
        cols.append(jnp.sum(d_out * map_a, axis=-1, keepdims=True))
        cols.append(jnp.sum(d_out * map_b, axis=-1, keepdims=True))
    rows = cols[0].shape[0]
    lane = lax.broadcasted_iota(jnp.int32, (rows, 128), 1)
    packed = jnp.zeros((rows, 128), jnp.float32)
    for at, col in enumerate(cols):
        packed = jnp.where(lane == at, col, packed)
    term_ref[...] = packed.T[: 2 * heads]


def block_grads(heads, groups, k_ref, v_ref, q_ref, d_ref, log_ref, term_ref, mix_ref, gq_ref, masked):
    per_group = heads // groups
    scale = HEAD_DIM ** (-0.5)
    outs_k, outs_v = [], []
    for g in range(groups):
        keys = [k_ref[:, (2 * g + m) * HEAD_DIM : (2 * g + m + 1) * HEAD_DIM] for m in range(2)]
        keys_t = [k.T for k in keys]
        vals = v_ref[:, g * V_DIM : (g + 1) * V_DIM]
        grad_k = [None, None]
        grad_v = None
        for h in range(g * per_group, (g + 1) * per_group):
            mix = mix_ref[h]
            d_h = d_ref[:, h * V_DIM : (h + 1) * V_DIM]
            d_attn = dot_nt(vals, d_h)
            qs, probs = [], []
            for m in range(2):
                at = 2 * h + m
                q = q_ref[:, at * HEAD_DIM : (at + 1) * HEAD_DIM]
                s = dot_nt(keys[m], q)
                p = jnp.exp2(s * (scale * LOG2E) - log_ref[at : at + 1, :] * LOG2E)
                if masked:
                    k_at = lax.broadcasted_iota(jnp.int32, p.shape, 0)
                    q_at = lax.broadcasted_iota(jnp.int32, p.shape, 1)
                    p = jnp.where(k_at <= q_at, p, 0.0)
                qs.append(q)
                probs.append(p)
            mixed = mix * probs[1]
            w = (probs[0] - mixed).astype(jnp.bfloat16)
            ds = [
                (probs[0] * (d_attn - term_ref[2 * h : 2 * h + 1, :])).astype(jnp.bfloat16),
                (mixed * (term_ref[2 * h + 1 : 2 * h + 2, :] - d_attn)).astype(jnp.bfloat16),
            ]
            for m in range(2):
                at = 2 * h + m
                gq_ref[at * HEAD_DIM : (at + 1) * HEAD_DIM, :] += dot_nn(keys_t[m], ds[m])
                gk = dot_nn(ds[m], qs[m])
                grad_k[m] = gk if grad_k[m] is None else grad_k[m] + gk
            gv = dot_nn(w, d_h)
            grad_v = gv if grad_v is None else grad_v + gv
        outs_k += [gk * scale for gk in grad_k]
        outs_v.append(grad_v)
    return outs_k, outs_v


def attend_kernel(
    n, tp_count, heads, groups,
    hidden_ref, weight_ref, values_ref, q_ref, mo_ref, og_ref, log_ref, gain_ref, mix_ref,
    gq_out, gk_out, gv_out, gw_out,
    d_ref, term_ref, gq_ref, kv_ref, acc_ref, side_out, side_in, down_out, up_in, hid_ref, gk_ref,
    kv_recv, kv_up_sem, kv_side_sem, side_send, side_recv, down_send, up_recv,
    hid_send, hid_pass, hid_recv, gk_recv, gk_up_sem, gk_down_sem, gk_side_sem,
):
    me = lax.axis_index("sp")
    outer = n // 2
    o, y = me // 2, me % 2
    has_up = o < outer - 1
    up, down, side = me + 2, me - 2, me + 1 - 2 * y

    def kv_copy(b, part, sems, target, src=None):
        return pltpu.make_async_remote_copy(
            src_ref=kv_ref.at[b, part] if src is None else src,
            dst_ref=kv_ref.at[b, part],
            send_sem=sems.at[b // 2, part],
            recv_sem=kv_recv.at[b, part],
            device_id={"sp": target},
        )

    def side_copy(ob, part):
        return pltpu.make_async_remote_copy(
            src_ref=side_out.at[ob, part],
            dst_ref=side_in.at[ob, part],
            send_sem=side_send.at[ob, part],
            recv_sem=side_recv.at[ob, part],
            device_id={"sp": side},
        )

    def down_copy(ob, part):
        return pltpu.make_async_remote_copy(
            src_ref=down_out.at[ob, part],
            dst_ref=up_in.at[ob, part],
            send_sem=down_send.at[ob, part],
            recv_sem=up_recv.at[ob, part],
            device_id={"sp": down},
        )

    tp_at = lax.axis_index("tp")
    rows = q_ref.shape[0]
    part_rows = rows // tp_count
    wide = hidden_ref.shape[1] // n
    own_cols = pl.ds(pl.multiple_of(me * wide, wide), wide)
    own_rows = pl.ds(pl.multiple_of(tp_at * part_rows, part_rows), part_rows)

    def hid_slice(dest):
        return pltpu.make_async_remote_copy(
            src_ref=hidden_ref.at[own_rows, pl.ds(pl.multiple_of(dest * wide, wide), wide)],
            dst_ref=hid_ref.at[tp_at, me],
            send_sem=hid_send,
            recv_sem=hid_recv.at[tp_at],
            device_id={"sp": dest},
        )

    def hid_forward(source, target):
        return pltpu.make_async_remote_copy(
            src_ref=hid_ref.at[source],
            dst_ref=hid_ref.at[source],
            send_sem=hid_pass.at[target],
            recv_sem=hid_recv.at[source],
            device_id={"tp": target},
        )

    def hid_start():
        @pl.loop(1, n)
        def _(k):
            hid_slice((me + k) % n).start()

    def hid_wait(sem):
        pieces = hid_ref.at[tp_at, pl.ds(0, n - 1)]
        pltpu.make_async_copy(pieces, pieces, sem).wait()

    def hid_relay():
        hid_wait(hid_recv.at[tp_at])

        @pl.loop(1, tp_count)
        def _(k):
            hid_forward(tp_at, (tp_at + k) % tp_count).start()

    def gk_copy(b, sems, target):
        return pltpu.make_async_remote_copy(
            src_ref=gk_ref.at[b],
            dst_ref=gk_ref.at[b],
            send_sem=sems.at[b // 2],
            recv_sem=gk_recv.at[b],
            device_id={"sp": target},
        )

    def gk_each(b, act):
        ob = b // 2

        @pl.when((ob <= o) & has_up)
        def _():
            act(gk_copy(b, gk_up_sem, up))

        @pl.when((ob >= o) & (o > 0))
        def _():
            act(gk_copy(b, gk_down_sem, down))

        act(gk_copy(b, gk_side_sem, side))

    def add_weight(b):
        block = jnp.concatenate([hid_ref[k, b] for k in range(tp_count)], axis=0)
        gw_out[...] += dot_tn(block, gk_ref[b])

    barrier = pltpu.get_barrier_semaphore()

    @pl.loop(1, n)
    def _(k):
        pl.semaphore_signal(barrier, inc=1, device_id={"sp": (me + k) % n})

    @pl.loop(1, tp_count)
    def _(k):
        pl.semaphore_signal(barrier, inc=1, device_id={"tp": (tp_at + k) % tp_count})

    pl.semaphore_wait(barrier, n + tp_count - 2)

    def start_own(part, src=None):
        @pl.when(has_up)
        def _():
            kv_copy(me, part, kv_up_sem, up, src).start()

        @pl.when(y == 0)
        def _():
            kv_copy(me, part, kv_side_sem, side, src).start()

    start_own(1, values_ref)
    kv_ref[me, 0] = dot_nn(hidden_ref[...], weight_ref[...]).astype(jnp.bfloat16)
    kv_ref[me, 1] = values_ref[...]
    start_own(0)
    hid_ref[tp_at, me] = hidden_ref[own_rows, own_cols]

    @pl.when(~has_up)
    def _():
        hid_start()

    head_terms(heads, og_ref, mo_ref, mix_ref, gain_ref, d_ref, term_ref)
    gw_out[...] = jnp.zeros_like(gw_out)
    gq_ref[...] = jnp.zeros_like(gq_ref)

    def grads(b, masked):
        return block_grads(
            heads, groups, kv_ref.at[b, 0], kv_ref.at[b, 1], q_ref, d_ref, log_ref, term_ref, mix_ref, gq_ref, masked
        )

    def store(ref, ob, pieces):
        for part in range(2):
            at = 0
            for piece in pieces[part]:
                ref[ob, part, :, at : at + piece.shape[1]] = piece.astype(ref.dtype)
                at += piece.shape[1]

    lag = jnp.where(has_up, o + 2, 2)

    @pl.loop(0, o + lag + 1)
    def _(t):
        @pl.when(t == 0)
        def _():
            store(acc_ref, o, grads(me, True))

        @pl.when((t > 0) & (t <= o))
        def _():
            b = me - 2 * t
            for part in (1, 0):
                kv_copy(b, part, kv_up_sem, up).wait_recv()

                @pl.when(has_up)
                def _():
                    kv_copy(b, part, kv_up_sem, up).start()

                kv_copy(b, part, kv_side_sem, side).start()
            store(acc_ref, o - t, grads(b, False))

        @pl.when((t > 0) & (t <= o + 1) & ((t > 1) | (y == 1)))
        def _():
            ob = o - t + 1
            b = 2 * ob + 1 - y
            for part in (1, 0):
                kv_copy(b, part, kv_side_sem, side).wait_recv()
            store(side_out, ob, grads(b, False))
            for part in range(2):
                side_copy(ob, part).start()

        @pl.when((t == o + 1) & has_up)
        def _():
            hid_start()

        @pl.when((t == o + 2) & has_up)
        def _():
            hid_relay()

        @pl.when(t >= lag)
        def _():
            ob = o - t + lag
            for part in range(2):
                @pl.when((ob < o) | (y == 0))
                def _():
                    side_copy(ob, part).wait_recv()
                    acc_ref[ob, part] += side_in[ob, part].astype(jnp.float32)

                @pl.when(has_up)
                def _():
                    down_copy(ob, part).wait_recv()
                    acc_ref[ob, part] += up_in[ob, part].astype(jnp.float32)

                if part == 0:
                    @pl.when(ob == o)
                    def _():
                        gk_ref[me] = acc_ref[o, 0].astype(jnp.bfloat16)
                        gk_each(me, lambda copy: copy.start())

                @pl.when(ob < o)
                def _():
                    down_out[ob, part] = acc_ref[ob, part].astype(jnp.bfloat16)
                    down_copy(ob, part).start()

        @pl.when(t == o + 1)
        def _():
            for at in range(2 * heads):
                cols = slice(at * HEAD_DIM, (at + 1) * HEAD_DIM)
                gq_out[:, cols] = (gq_ref[cols, :] * HEAD_DIM ** (-0.5)).T.astype(gq_out.dtype)

    @pl.when(~has_up)
    def _():
        hid_relay()

    gk_out[...] = gk_ref[me]
    gv_out[...] = acc_ref[o, 1].astype(gv_out.dtype)

    @pl.loop(1, tp_count)
    def _(k):
        hid_forward((tp_at + k) % tp_count, tp_at).wait_recv()

    add_weight(me)

    @pl.loop(0, outer)
    def _(k):
        b = 2 * (outer - 1 - k) + y

        @pl.when(b != me)
        def _():
            gk_copy(b, gk_side_sem, side).wait_recv()
            gk_each(b, lambda copy: copy.start())
            add_weight(b)

    @pl.loop(0, outer)
    def _(k):
        b = 2 * (outer - 1 - k) + 1 - y
        gk_copy(b, gk_side_sem, side).wait_recv()
        add_weight(b)

    hid_wait(hid_send)

    @pl.loop(1, tp_count)
    def _(k):
        hid_forward(tp_at, (tp_at + k) % tp_count).wait_send()

    @pl.loop(0, outer)
    def _(ob):
        gk_each(2 * ob + y, lambda copy: copy.wait_send())

    @pl.loop(0, o + 1)
    def _(ob):
        for part in range(2):
            @pl.when(has_up)
            def _():
                kv_copy(2 * ob + y, part, kv_up_sem, up).wait_send()

            @pl.when((ob < o) | (y == 0))
            def _():
                kv_copy(2 * ob + y, part, kv_side_sem, side).wait_send()

            @pl.when((ob < o) | (y == 1))
            def _():
                side_copy(ob, part).wait_send()

            @pl.when(ob < o)
            def _():
                down_copy(ob, part).wait_send()


def on_device(n, tp_count, hidden, key_weight, queries, values, map_out, log_sums, out_grad, mixing, out_gain):
    rows = queries.shape[0]
    heads = mixing.shape[0]
    width = values.shape[1]
    groups = width // V_DIM
    outer = n // 2
    vm = pl.BlockSpec(memory_space=VMEM)
    hops = pltpu.SemaphoreType.DMA((outer, 2))
    return pl.pallas_call(
        functools.partial(attend_kernel, n, tp_count, heads, groups),
        out_shape=(
            jax.ShapeDtypeStruct(queries.shape, jnp.bfloat16),
            jax.ShapeDtypeStruct((rows, width), jnp.bfloat16),
            jax.ShapeDtypeStruct((rows, width), jnp.bfloat16),
            jax.ShapeDtypeStruct((hidden.shape[1] // n, width), jnp.float32),
        ),
        in_specs=[vm] * 8 + [pl.BlockSpec(memory_space=pltpu.SMEM)],
        out_specs=(vm, vm, vm, vm),
        scratch_shapes=[
            VMEM((rows, heads * V_DIM), jnp.bfloat16),
            VMEM((2 * heads, rows), jnp.float32),
            VMEM((2 * heads * HEAD_DIM, rows), jnp.float32),
            VMEM((n, 2, rows, width), jnp.bfloat16),
            VMEM((outer, 2, rows, width), jnp.float32),
        ]
        + [VMEM((outer, 2, rows, width), jnp.bfloat16)] * 4
        + [
            VMEM((tp_count, n, rows // tp_count, hidden.shape[1] // n), jnp.bfloat16),
            VMEM((n, rows, width), jnp.bfloat16),
        ]
        + [pltpu.SemaphoreType.DMA((n, 2))]
        + [hops] * 6
        + [pltpu.SemaphoreType.DMA]
        + [pltpu.SemaphoreType.DMA((size,)) for size in (tp_count, tp_count, n, outer, outer, outer)],
        compiler_params=pltpu.CompilerParams(
            vmem_limit_bytes=60 * 2**20, collective_id=0, has_side_effects=True
        ),
        cost_estimate=pl.CostEstimate(flops=5 * 10**9, bytes_accessed=10**7, transcendentals=0),
    )(hidden, key_weight, values, queries, map_out, out_grad, log_sums, out_gain.reshape(1, V_DIM), mixing)


def solution(mesh):
    placed = (
        P("sp", None),
        P(None, "tp"),
        P("sp", "tp"),
        P("sp", "tp"),
        P("sp", "tp"),
        P("tp", "sp"),
        P("sp", "tp"),
        P("tp"),
        P(),
    )
    return jax.shard_map(
        functools.partial(on_device, mesh.shape["sp"], mesh.shape["tp"]),
        mesh=mesh,
        in_specs=placed,
        out_specs=(P("sp", "tp"), P("sp", "tp"), P("sp", "tp"), P("sp", "tp")),
        check_vma=False,
    )
```

```python
import functools
import math

import jax
import jax.numpy as jnp
from jax import lax
from jax.experimental import pallas as pl
from jax.experimental.pallas import tpu as pltpu
from jax.sharding import PartitionSpec as P

HEAD_DIM = 128
V_DIM = 256
OUT_SCALE = 0.8
NORM_EPS = 1e-06
LOG2E = math.log2(math.e)
VMEM = pltpu.VMEM


def dot_nn(a, b):
    return lax.dot_general(a, b, (((1,), (0,)), ((), ())), preferred_element_type=jnp.float32)


def dot_nt(a, b):
    return lax.dot_general(a, b, (((1,), (1,)), ((), ())), preferred_element_type=jnp.float32)


def dot_tn(a, b):
    return lax.dot_general(a, b, (((0,), (0,)), ((), ())), preferred_element_type=jnp.float32)


def head_terms(heads, og_ref, mo_ref, mix_ref, gain_ref, d_ref, term_ref):
    gain = gain_ref[...] * OUT_SCALE
    cols = []
    for h in range(heads):
        v_cols = pl.ds(h * V_DIM, V_DIM)
        map_a = mo_ref[:, pl.ds(2 * h * V_DIM, V_DIM)].astype(jnp.float32)
        map_b = mo_ref[:, pl.ds((2 * h + 1) * V_DIM, V_DIM)].astype(jnp.float32)
        pre = map_a - mix_ref[h] * map_b
        inv = lax.rsqrt(jnp.mean(pre * pre, axis=-1, keepdims=True) + NORM_EPS)
        up = og_ref[:, v_cols].astype(jnp.float32) * gain
        d_out = inv * (up - pre * (inv * inv * jnp.mean(up * pre, axis=-1, keepdims=True)))
        d_ref[:, v_cols] = d_out.astype(jnp.bfloat16)
        cols.append(jnp.sum(d_out * map_a, axis=-1, keepdims=True))
        cols.append(jnp.sum(d_out * map_b, axis=-1, keepdims=True))
    rows = cols[0].shape[0]
    lane = lax.broadcasted_iota(jnp.int32, (rows, 128), 1)
    packed = jnp.zeros((rows, 128), jnp.float32)
    for at, col in enumerate(cols):
        packed = jnp.where(lane == at, col, packed)
    term_ref[...] = packed.T[: 2 * heads]


def block_grads(heads, groups, k_ref, v_ref, q_ref, d_ref, log_ref, term_ref, mix_ref, gq_ref, masked):
    per_group = heads // groups
    scale = HEAD_DIM ** (-0.5)
    outs_k, outs_v = [], []
    for g in range(groups):
        keys = [k_ref[:, (2 * g + m) * HEAD_DIM : (2 * g + m + 1) * HEAD_DIM] for m in range(2)]
        keys_t = [k.T for k in keys]
        vals = v_ref[:, g * V_DIM : (g + 1) * V_DIM]
        grad_k = [None, None]
        grad_v = None
        for h in range(g * per_group, (g + 1) * per_group):
            mix = mix_ref[h]
            d_h = d_ref[:, h * V_DIM : (h + 1) * V_DIM]
            d_attn = dot_nt(vals, d_h)
            qs, probs = [], []
            for m in range(2):
                at = 2 * h + m
                q = q_ref[:, at * HEAD_DIM : (at + 1) * HEAD_DIM]
                s = dot_nt(keys[m], q)
                p = jnp.exp2(s * (scale * LOG2E) - log_ref[at : at + 1, :] * LOG2E)
                if masked:
                    k_at = lax.broadcasted_iota(jnp.int32, p.shape, 0)
                    q_at = lax.broadcasted_iota(jnp.int32, p.shape, 1)
                    p = jnp.where(k_at <= q_at, p, 0.0)
                qs.append(q)
                probs.append(p)
            mixed = mix * probs[1]
            w = (probs[0] - mixed).astype(jnp.bfloat16)
            ds = [
                (probs[0] * (d_attn - term_ref[2 * h : 2 * h + 1, :])).astype(jnp.bfloat16),
                (mixed * (term_ref[2 * h + 1 : 2 * h + 2, :] - d_attn)).astype(jnp.bfloat16),
            ]
            for m in range(2):
                at = 2 * h + m
                gq_ref[at * HEAD_DIM : (at + 1) * HEAD_DIM, :] += dot_nn(keys_t[m], ds[m])
                gk = dot_nn(ds[m], qs[m])
                grad_k[m] = gk if grad_k[m] is None else grad_k[m] + gk
            gv = dot_nn(w, d_h)
            grad_v = gv if grad_v is None else grad_v + gv
        outs_k += [gk * scale for gk in grad_k]
        outs_v.append(grad_v)
    return outs_k, outs_v


def attend_kernel(
    n, tp_count, heads, groups,
    hidden_ref, weight_ref, values_ref, q_ref, mo_ref, og_ref, log_ref, gain_ref, mix_ref,
    gq_out, gk_out, gv_out, gw_out,
    d_ref, term_ref, gq_ref, kv_ref, acc_ref, side_out, side_in, down_out, up_in, hid_ref, gk_ref,
    kv_recv, kv_up_sem, kv_side_sem, side_send, side_recv, down_send, up_recv,
    hid_send, hid_pass, hid_recv, gk_recv, gk_up_sem, gk_down_sem, gk_side_sem,
):
    me = lax.axis_index("sp")
    outer = n // 2
    o, y = me // 2, me % 2
    has_up = o < outer - 1
    up, down, side = me + 2, me - 2, me + 1 - 2 * y

    def kv_copy(b, part, sems, target, src=None):
        return pltpu.make_async_remote_copy(
            src_ref=kv_ref.at[b, part] if src is None else src,
            dst_ref=kv_ref.at[b, part],
            send_sem=sems.at[b // 2, part],
            recv_sem=kv_recv.at[b, part],
            device_id={"sp": target},
        )

    def side_copy(ob, part):
        return pltpu.make_async_remote_copy(
            src_ref=side_out.at[ob, part],
            dst_ref=side_in.at[ob, part],
            send_sem=side_send.at[ob, part],
            recv_sem=side_recv.at[ob, part],
            device_id={"sp": side},
        )

    def down_copy(ob, part):
        return pltpu.make_async_remote_copy(
            src_ref=down_out.at[ob, part],
            dst_ref=up_in.at[ob, part],
            send_sem=down_send.at[ob, part],
            recv_sem=up_recv.at[ob, part],
            device_id={"sp": down},
        )

    tp_at = lax.axis_index("tp")
    rows = q_ref.shape[0]
    part_rows = rows // tp_count
    wide = hidden_ref.shape[1] // n
    own_cols = pl.ds(pl.multiple_of(me * wide, wide), wide)
    own_rows = pl.ds(pl.multiple_of(tp_at * part_rows, part_rows), part_rows)

    def hid_slice(dest):
        return pltpu.make_async_remote_copy(
            src_ref=hidden_ref.at[own_rows, pl.ds(pl.multiple_of(dest * wide, wide), wide)],
            dst_ref=hid_ref.at[tp_at, me],
            send_sem=hid_send,
            recv_sem=hid_recv.at[tp_at],
            device_id={"sp": dest},
        )

    def hid_forward(source, target):
        return pltpu.make_async_remote_copy(
            src_ref=hid_ref.at[source],
            dst_ref=hid_ref.at[source],
            send_sem=hid_pass.at[target],
            recv_sem=hid_recv.at[source],
            device_id={"tp": target},
        )

    def hid_start():
        @pl.loop(1, n)
        def _(k):
            hid_slice((me + k) % n).start()

    def hid_wait(sem):
        pieces = hid_ref.at[tp_at, pl.ds(0, n - 1)]
        pltpu.make_async_copy(pieces, pieces, sem).wait()

    def hid_relay():
        hid_wait(hid_recv.at[tp_at])

        @pl.loop(1, tp_count)
        def _(k):
            hid_forward(tp_at, (tp_at + k) % tp_count).start()

    def gk_copy(b, sems, target):
        return pltpu.make_async_remote_copy(
            src_ref=gk_ref.at[b],
            dst_ref=gk_ref.at[b],
            send_sem=sems.at[b // 2],
            recv_sem=gk_recv.at[b],
            device_id={"sp": target},
        )

    def gk_each(b, act):
        ob = b // 2

        @pl.when((ob <= o) & has_up)
        def _():
            act(gk_copy(b, gk_up_sem, up))

        @pl.when((ob >= o) & (o > 0))
        def _():
            act(gk_copy(b, gk_down_sem, down))

        act(gk_copy(b, gk_side_sem, side))

    def add_weight(b):
        block = jnp.concatenate([hid_ref[k, b] for k in range(tp_count)], axis=0)
        gw_out[...] += dot_tn(block, gk_ref[b])

    barrier = pltpu.get_barrier_semaphore()

    @pl.loop(1, n)
    def _(k):
        pl.semaphore_signal(barrier, inc=1, device_id={"sp": (me + k) % n})

    @pl.loop(1, tp_count)
    def _(k):
        pl.semaphore_signal(barrier, inc=1, device_id={"tp": (tp_at + k) % tp_count})

    pl.semaphore_wait(barrier, n + tp_count - 2)

    def start_own(part, src=None):
        @pl.when(has_up)
        def _():
            kv_copy(me, part, kv_up_sem, up, src).start()

        @pl.when(y == 0)
        def _():
            kv_copy(me, part, kv_side_sem, side, src).start()

    start_own(1, values_ref)
    kv_ref[me, 0] = dot_nn(hidden_ref[...], weight_ref[...]).astype(jnp.bfloat16)
    kv_ref[me, 1] = values_ref[...]
    start_own(0)
    hid_ref[tp_at, me] = hidden_ref[own_rows, own_cols]

    @pl.when(~has_up)
    def _():
        hid_start()

    head_terms(heads, og_ref, mo_ref, mix_ref, gain_ref, d_ref, term_ref)
    gw_out[...] = jnp.zeros_like(gw_out)
    gq_ref[...] = jnp.zeros_like(gq_ref)

    def grads(b, masked):
        return block_grads(
            heads, groups, kv_ref.at[b, 0], kv_ref.at[b, 1], q_ref, d_ref, log_ref, term_ref, mix_ref, gq_ref, masked
        )

    def store(ref, ob, pieces):
        for part in range(2):
            at = 0
            for piece in pieces[part]:
                ref[ob, part, :, at : at + piece.shape[1]] = piece.astype(ref.dtype)
                at += piece.shape[1]

    lag = jnp.where(has_up, o + 2, 2)

    @pl.loop(0, o + lag + 1)
    def _(t):
        @pl.when(t == 0)
        def _():
            store(acc_ref, o, grads(me, True))

        @pl.when((t > 0) & (t <= o))
        def _():
            b = me - 2 * t
            for part in (1, 0):
                kv_copy(b, part, kv_up_sem, up).wait_recv()

                @pl.when(has_up)
                def _():
                    kv_copy(b, part, kv_up_sem, up).start()

                kv_copy(b, part, kv_side_sem, side).start()
            store(acc_ref, o - t, grads(b, False))

        @pl.when((t > 0) & (t <= o + 1) & ((t > 1) | (y == 1)))
        def _():
            ob = o - t + 1
            b = 2 * ob + 1 - y
            for part in (1, 0):
                kv_copy(b, part, kv_side_sem, side).wait_recv()
            store(side_out, ob, grads(b, False))
            for part in range(2):
                side_copy(ob, part).start()

        @pl.when((t == o + 1) & has_up)
        def _():
            hid_start()

        @pl.when((t == o + 2) & has_up)
        def _():
            hid_relay()

        @pl.when(t >= lag)
        def _():
            ob = o - t + lag
            for part in range(2):
                @pl.when((ob < o) | (y == 0))
                def _():
                    side_copy(ob, part).wait_recv()
                    acc_ref[ob, part] += side_in[ob, part].astype(jnp.float32)

                @pl.when(has_up)
                def _():
                    down_copy(ob, part).wait_recv()
                    acc_ref[ob, part] += up_in[ob, part].astype(jnp.float32)

                if part == 0:
                    @pl.when(ob == o)
                    def _():
                        gk_ref[me] = acc_ref[o, 0].astype(jnp.bfloat16)
                        gk_each(me, lambda copy: copy.start())

                @pl.when(ob < o)
                def _():
                    down_out[ob, part] = acc_ref[ob, part].astype(jnp.bfloat16)
                    down_copy(ob, part).start()

        @pl.when(t == o + 1)
        def _():
            for at in range(2 * heads):
                cols = slice(at * HEAD_DIM, (at + 1) * HEAD_DIM)
                gq_out[:, cols] = (gq_ref[cols, :] * HEAD_DIM ** (-0.5)).T.astype(gq_out.dtype)

    @pl.when(~has_up)
    def _():
        hid_relay()

    gk_out[...] = gk_ref[me]
    gv_out[...] = acc_ref[o, 1].astype(gv_out.dtype)

    @pl.loop(1, tp_count)
    def _(k):
        hid_forward((tp_at + k) % tp_count, tp_at).wait_recv()

    add_weight(me)

    @pl.loop(0, outer)
    def _(k):
        b = 2 * (outer - 1 - k) + y

        @pl.when(b != me)
        def _():
            gk_copy(b, gk_side_sem, side).wait_recv()
            gk_each(b, lambda copy: copy.start())
            add_weight(b)

    @pl.loop(0, outer)
    def _(k):
        b = 2 * (outer - 1 - k) + 1 - y
        gk_copy(b, gk_side_sem, side).wait_recv()
        add_weight(b)

    hid_wait(hid_send)

    @pl.loop(1, tp_count)
    def _(k):
        hid_forward(tp_at, (tp_at + k) % tp_count).wait_send()

    @pl.loop(0, outer)
    def _(ob):
        gk_each(2 * ob + y, lambda copy: copy.wait_send())

    @pl.loop(0, o + 1)
    def _(ob):
        for part in range(2):
            @pl.when(has_up)
            def _():
                kv_copy(2 * ob + y, part, kv_up_sem, up).wait_send()

            @pl.when((ob < o) | (y == 0))
            def _():
                kv_copy(2 * ob + y, part, kv_side_sem, side).wait_send()

            @pl.when((ob < o) | (y == 1))
            def _():
                side_copy(ob, part).wait_send()

            @pl.when(ob < o)
            def _():
                down_copy(ob, part).wait_send()


def write_kernel(*refs):
    for src, dst in zip(refs[:4], refs[4:]):
        dst[...] = src[...]


def on_device(n, tp_count, hidden, key_weight, queries, values, map_out, log_sums, out_grad, mixing, out_gain):
    rows = queries.shape[0]
    heads = mixing.shape[0]
    width = values.shape[1]
    groups = width // V_DIM
    outer = n // 2
    vm = pl.BlockSpec(memory_space=VMEM)
    hops = pltpu.SemaphoreType.DMA((outer, 2))
    results = pl.pallas_call(
        functools.partial(attend_kernel, n, tp_count, heads, groups),
        out_shape=(
            jax.ShapeDtypeStruct(queries.shape, jnp.bfloat16),
            jax.ShapeDtypeStruct((rows, width), jnp.bfloat16),
            jax.ShapeDtypeStruct((rows, width), jnp.bfloat16),
            jax.ShapeDtypeStruct((hidden.shape[1] // n, width), jnp.float32),
        ),
        in_specs=[vm] * 8 + [pl.BlockSpec(memory_space=pltpu.SMEM)],
        out_specs=(vm, vm, vm, vm),
        scratch_shapes=[
            VMEM((rows, heads * V_DIM), jnp.bfloat16),
            VMEM((2 * heads, rows), jnp.float32),
            VMEM((2 * heads * HEAD_DIM, rows), jnp.float32),
            VMEM((n, 2, rows, width), jnp.bfloat16),
            VMEM((outer, 2, rows, width), jnp.float32),
        ]
        + [VMEM((outer, 2, rows, width), jnp.bfloat16)] * 4
        + [
            VMEM((tp_count, n, rows // tp_count, hidden.shape[1] // n), jnp.bfloat16),
            VMEM((n, rows, width), jnp.bfloat16),
        ]
        + [pltpu.SemaphoreType.DMA((n, 2))]
        + [hops] * 6
        + [pltpu.SemaphoreType.DMA]
        + [pltpu.SemaphoreType.DMA((size,)) for size in (tp_count, tp_count, n, outer, outer, outer)],
        compiler_params=pltpu.CompilerParams(
            vmem_limit_bytes=60 * 2**20, collective_id=0, has_side_effects=True
        ),
        cost_estimate=pl.CostEstimate(flops=5 * 10**9, bytes_accessed=10**7, transcendentals=0),
    )(hidden, key_weight, values, queries, map_out, out_grad, log_sums, out_gain.reshape(1, V_DIM), mixing)
    return pl.pallas_call(
        write_kernel,
        out_shape=tuple(jax.ShapeDtypeStruct(r.shape, r.dtype) for r in results),
        in_specs=[vm] * 4,
        out_specs=(vm,) * 4,
        cost_estimate=pl.CostEstimate(flops=10**6, bytes_accessed=4 * 10**6, transcendentals=0),
    )(*results)


def solution(mesh):
    placed = (
        P("sp", None),
        P(None, "tp"),
        P("sp", "tp"),
        P("sp", "tp"),
        P("sp", "tp"),
        P("tp", "sp"),
        P("sp", "tp"),
        P("tp"),
        P(),
    )
    return jax.shard_map(
        functools.partial(on_device, mesh.shape["sp"], mesh.shape["tp"]),
        mesh=mesh,
        in_specs=placed,
        out_specs=(P("sp", "tp"), P("sp", "tp"), P("sp", "tp"), P("sp", "tp")),
        check_vma=False,
    )
```

```python
import functools
import math

import jax
import jax.numpy as jnp
from jax import lax
from jax.experimental import pallas as pl
from jax.experimental.pallas import tpu as pltpu
from jax.sharding import PartitionSpec as P

HEAD_DIM = 128
V_DIM = 256
OUT_SCALE = 0.8
NORM_EPS = 1e-06
LOG2E = math.log2(math.e)
VMEM = pltpu.VMEM


def dot_nn(a, b):
    return lax.dot_general(a, b, (((1,), (0,)), ((), ())), preferred_element_type=jnp.float32)


def dot_nt(a, b):
    return lax.dot_general(a, b, (((1,), (1,)), ((), ())), preferred_element_type=jnp.float32)


def dot_tn(a, b):
    return lax.dot_general(a, b, (((0,), (0,)), ((), ())), preferred_element_type=jnp.float32)


def head_terms(heads, og_ref, mo_ref, mix_ref, gain_ref, d_ref, term_ref):
    gain = gain_ref[...] * OUT_SCALE
    cols = []
    for h in range(heads):
        v_cols = pl.ds(h * V_DIM, V_DIM)
        map_a = mo_ref[:, pl.ds(2 * h * V_DIM, V_DIM)].astype(jnp.float32)
        map_b = mo_ref[:, pl.ds((2 * h + 1) * V_DIM, V_DIM)].astype(jnp.float32)
        pre = map_a - mix_ref[h] * map_b
        inv = lax.rsqrt(jnp.mean(pre * pre, axis=-1, keepdims=True) + NORM_EPS)
        up = og_ref[:, v_cols].astype(jnp.float32) * gain
        d_out = inv * (up - pre * (inv * inv * jnp.mean(up * pre, axis=-1, keepdims=True)))
        d_ref[:, v_cols] = d_out.astype(jnp.bfloat16)
        cols.append(jnp.sum(d_out * map_a, axis=-1, keepdims=True))
        cols.append(jnp.sum(d_out * map_b, axis=-1, keepdims=True))
    rows = cols[0].shape[0]
    lane = lax.broadcasted_iota(jnp.int32, (rows, 128), 1)
    packed = jnp.zeros((rows, 128), jnp.float32)
    for at, col in enumerate(cols):
        packed = jnp.where(lane == at, col, packed)
    term_ref[...] = packed.T[: 2 * heads]


def block_grads(heads, groups, k_ref, v_ref, q_ref, d_ref, log_ref, term_ref, mix_ref, gq_ref, masked):
    per_group = heads // groups
    scale = HEAD_DIM ** (-0.5)
    outs_k, outs_v = [], []
    for g in range(groups):
        keys = [k_ref[:, (2 * g + m) * HEAD_DIM : (2 * g + m + 1) * HEAD_DIM] for m in range(2)]
        keys_t = [k.T for k in keys]
        vals = v_ref[:, g * V_DIM : (g + 1) * V_DIM]
        grad_k = [None, None]
        grad_v = None
        for h in range(g * per_group, (g + 1) * per_group):
            mix = mix_ref[h]
            d_h = d_ref[:, h * V_DIM : (h + 1) * V_DIM]
            d_attn = dot_nt(vals, d_h)
            qs, probs = [], []
            for m in range(2):
                at = 2 * h + m
                q = q_ref[:, at * HEAD_DIM : (at + 1) * HEAD_DIM]
                s = dot_nt(keys[m], q)
                p = jnp.exp2(s * (scale * LOG2E) - log_ref[at : at + 1, :] * LOG2E)
                if masked:
                    k_at = lax.broadcasted_iota(jnp.int32, p.shape, 0)
                    q_at = lax.broadcasted_iota(jnp.int32, p.shape, 1)
                    p = jnp.where(k_at <= q_at, p, 0.0)
                qs.append(q)
                probs.append(p)
            mixed = mix * probs[1]
            w = (probs[0] - mixed).astype(jnp.bfloat16)
            ds = [
                (probs[0] * (d_attn - term_ref[2 * h : 2 * h + 1, :])).astype(jnp.bfloat16),
                (mixed * (term_ref[2 * h + 1 : 2 * h + 2, :] - d_attn)).astype(jnp.bfloat16),
            ]
            for m in range(2):
                at = 2 * h + m
                gq_ref[at * HEAD_DIM : (at + 1) * HEAD_DIM, :] += dot_nn(keys_t[m], ds[m])
                gk = dot_nn(ds[m], qs[m])
                grad_k[m] = gk if grad_k[m] is None else grad_k[m] + gk
            gv = dot_nn(w, d_h)
            grad_v = gv if grad_v is None else grad_v + gv
        outs_k += [gk * scale for gk in grad_k]
        outs_v.append(grad_v)
    return outs_k, outs_v


def attend_kernel(
    n, tp_count, heads, groups,
    hidden_ref, weight_ref, values_ref, q_ref, mo_ref, og_ref, log_ref, gain_ref, mix_ref,
    gq_out, gk_out, gv_out, gw_out,
    d_ref, term_ref, gq_ref, kv_ref, acc_ref, side_out, side_in, down_out, up_in, up_side, hid_ref, gk_ref,
    kv_recv, kv_up_sem, kv_side_sem, side_send, side_recv, down_send, up_recv, cross_send, cross_recv,
    hid_send, hid_pass, hid_recv, gk_recv, gk_up_sem, gk_down_sem, gk_side_sem,
):
    me = lax.axis_index("sp")
    outer = n // 2
    o, y = me // 2, me % 2
    has_up = o < outer - 1
    up, down, side = me + 2, me - 2, me + 1 - 2 * y

    def kv_copy(b, part, sems, target, src=None):
        return pltpu.make_async_remote_copy(
            src_ref=kv_ref.at[b, part] if src is None else src,
            dst_ref=kv_ref.at[b, part],
            send_sem=sems.at[b, part],
            recv_sem=kv_recv.at[b, part],
            device_id={"sp": target},
        )

    def side_copy(ob, part):
        return pltpu.make_async_remote_copy(
            src_ref=side_out.at[ob, part],
            dst_ref=side_in.at[ob, part],
            send_sem=side_send.at[ob, part],
            recv_sem=side_recv.at[ob, part],
            device_id={"sp": side},
        )

    def down_copy(ob, part):
        return pltpu.make_async_remote_copy(
            src_ref=down_out.at[ob, part],
            dst_ref=up_in.at[ob, part],
            send_sem=down_send.at[ob, part],
            recv_sem=up_recv.at[ob, part],
            device_id={"sp": down},
        )

    def cross_copy(ob):
        return pltpu.make_async_remote_copy(
            src_ref=side_out.at[ob, 1],
            dst_ref=up_side.at[ob],
            send_sem=cross_send.at[ob],
            recv_sem=cross_recv.at[ob],
            device_id={"sp": down},
        )

    tp_at = lax.axis_index("tp")
    rows = q_ref.shape[0]
    part_rows = rows // tp_count
    wide = hidden_ref.shape[1] // n
    own_cols = pl.ds(pl.multiple_of(me * wide, wide), wide)
    own_rows = pl.ds(pl.multiple_of(tp_at * part_rows, part_rows), part_rows)

    def hid_slice(dest):
        return pltpu.make_async_remote_copy(
            src_ref=hidden_ref.at[own_rows, pl.ds(pl.multiple_of(dest * wide, wide), wide)],
            dst_ref=hid_ref.at[tp_at, me],
            send_sem=hid_send,
            recv_sem=hid_recv.at[tp_at],
            device_id={"sp": dest},
        )

    def hid_forward(source, target):
        return pltpu.make_async_remote_copy(
            src_ref=hid_ref.at[source],
            dst_ref=hid_ref.at[source],
            send_sem=hid_pass.at[target],
            recv_sem=hid_recv.at[source],
            device_id={"tp": target},
        )

    def hid_start():
        @pl.loop(1, n)
        def _(k):
            hid_slice((me + k) % n).start()

    def hid_wait(sem):
        pieces = hid_ref.at[tp_at, pl.ds(0, n - 1)]
        pltpu.make_async_copy(pieces, pieces, sem).wait()

    def hid_relay():
        hid_wait(hid_recv.at[tp_at])

        @pl.loop(1, tp_count)
        def _(k):
            hid_forward(tp_at, (tp_at + k) % tp_count).start()

    def gk_copy(b, sems, target):
        return pltpu.make_async_remote_copy(
            src_ref=gk_ref.at[b],
            dst_ref=gk_ref.at[b],
            send_sem=sems.at[b // 2],
            recv_sem=gk_recv.at[b],
            device_id={"sp": target},
        )

    def gk_each(b, act):
        ob = b // 2

        @pl.when((ob <= o) & has_up)
        def _():
            act(gk_copy(b, gk_up_sem, up))

        @pl.when((ob >= o) & (o > 0))
        def _():
            act(gk_copy(b, gk_down_sem, down))

        act(gk_copy(b, gk_side_sem, side))

    def add_weight(b):
        block = jnp.concatenate([hid_ref[k, b] for k in range(tp_count)], axis=0)
        gw_out[...] += dot_tn(block, gk_ref[b])

    barrier = pltpu.get_barrier_semaphore()

    @pl.loop(1, n)
    def _(k):
        pl.semaphore_signal(barrier, inc=1, device_id={"sp": (me + k) % n})

    @pl.loop(1, tp_count)
    def _(k):
        pl.semaphore_signal(barrier, inc=1, device_id={"tp": (tp_at + k) % tp_count})

    pl.semaphore_wait(barrier, n + tp_count - 2)

    def start_own(part, src=None):
        @pl.when(has_up)
        def _():
            kv_copy(me, part, kv_up_sem, up, src).start()

        @pl.when((y == 0) | (has_up & (part == 1)))
        def _():
            kv_copy(me, part, kv_side_sem, side, src).start()

    start_own(1, values_ref)
    kv_ref[me, 0] = dot_nn(hidden_ref[...], weight_ref[...]).astype(jnp.bfloat16)
    kv_ref[me, 1] = values_ref[...]
    start_own(0)
    hid_ref[tp_at, me] = hidden_ref[own_rows, own_cols]

    @pl.when(~has_up)
    def _():
        hid_start()

    head_terms(heads, og_ref, mo_ref, mix_ref, gain_ref, d_ref, term_ref)
    gw_out[...] = jnp.zeros_like(gw_out)
    gq_ref[...] = jnp.zeros_like(gq_ref)

    def grads(b, masked):
        return block_grads(
            heads, groups, kv_ref.at[b, 0], kv_ref.at[b, 1], q_ref, d_ref, log_ref, term_ref, mix_ref, gq_ref, masked
        )

    def store(ref, ob, pieces):
        for part in range(2):
            at = 0
            for piece in pieces[part]:
                ref[ob, part, :, at : at + piece.shape[1]] = piece.astype(ref.dtype)
                at += piece.shape[1]

    lag = jnp.where(has_up, o + 2, 2)

    @pl.loop(0, o + lag + 1)
    def _(t):
        @pl.when(t == 0)
        def _():
            store(acc_ref, o, grads(me, True))

        @pl.when((t > 0) & (t <= o))
        def _():
            b = me - 2 * t
            for part in (1, 0):
                kv_copy(b, part, kv_up_sem, up).wait_recv()

                @pl.when(has_up)
                def _():
                    kv_copy(b, part, kv_up_sem, up).start()

                if part == 0:
                    kv_copy(b, part, kv_side_sem, side).start()
            store(acc_ref, o - t, grads(b, False))

        @pl.when((t > 0) & (t <= o + 1) & ((t > 1) | (y == 1) | has_up))
        def _():
            ob = o - t + 1
            b = 2 * ob + 1 - y
            kv_copy(b, 1, kv_side_sem, side).wait_recv()

            @pl.when(has_up)
            def _():
                kv_copy(b, 1, kv_up_sem, up).start()

            @pl.when((t > 1) | (y == 1))
            def _():
                kv_copy(b, 0, kv_side_sem, side).wait_recv()
                store(side_out, ob, grads(b, False))
                side_copy(ob, 0).start()

        @pl.when((t == o + 1) & has_up)
        def _():
            hid_start()

        @pl.when((t == o + 2) & has_up)
        def _():
            hid_relay()

        @pl.when(t >= lag)
        def _():
            ob = o - t + lag
            for part in range(2):
                if part == 1:
                    @pl.when(has_up)
                    def _():
                        cross_copy(ob).wait_recv()

                        @pl.when((ob < o) | (y == 1))
                        def _():
                            total = side_out[ob, 1].astype(jnp.float32) + up_side[ob].astype(jnp.float32)
                            side_out[ob, 1] = total.astype(jnp.bfloat16)

                        @pl.when((ob == o) & (y == 0))
                        def _():
                            side_out[ob, 1] = up_side[ob]

                    @pl.when(ob < o)
                    def _():
                        cross_copy(ob).start()

                    @pl.when((ob == o) & ((y == 1) | has_up))
                    def _():
                        side_copy(ob, 1).start()

                @pl.when(((ob < o) | (y == 0)) if part == 0 else ((ob == o) & ((y == 0) | has_up)))
                def _():
                    side_copy(ob, part).wait_recv()
                    acc_ref[ob, part] += side_in[ob, part].astype(jnp.float32)

                @pl.when(has_up)
                def _():
                    down_copy(ob, part).wait_recv()
                    acc_ref[ob, part] += up_in[ob, part].astype(jnp.float32)

                if part == 0:
                    @pl.when(ob == o)
                    def _():
                        gk_ref[me] = acc_ref[o, 0].astype(jnp.bfloat16)
                        gk_each(me, lambda copy: copy.start())

                @pl.when(ob < o)
                def _():
                    down_out[ob, part] = acc_ref[ob, part].astype(jnp.bfloat16)
                    down_copy(ob, part).start()

        @pl.when(t == o + 1)
        def _():
            for at in range(2 * heads):
                cols = slice(at * HEAD_DIM, (at + 1) * HEAD_DIM)
                gq_out[:, cols] = (gq_ref[cols, :] * HEAD_DIM ** (-0.5)).T.astype(gq_out.dtype)

    @pl.when(~has_up)
    def _():
        hid_relay()

    gk_out[...] = gk_ref[me]
    gv_out[...] = acc_ref[o, 1].astype(gv_out.dtype)

    @pl.loop(1, tp_count)
    def _(k):
        hid_forward((tp_at + k) % tp_count, tp_at).wait_recv()

    add_weight(me)

    @pl.loop(0, outer)
    def _(k):
        b = 2 * (outer - 1 - k) + y

        @pl.when(b != me)
        def _():
            gk_copy(b, gk_side_sem, side).wait_recv()
            gk_each(b, lambda copy: copy.start())
            add_weight(b)

    @pl.loop(0, outer)
    def _(k):
        b = 2 * (outer - 1 - k) + 1 - y
        gk_copy(b, gk_side_sem, side).wait_recv()
        add_weight(b)

    hid_wait(hid_send)

    @pl.loop(1, tp_count)
    def _(k):
        hid_forward(tp_at, (tp_at + k) % tp_count).wait_send()

    @pl.loop(0, outer)
    def _(ob):
        gk_each(2 * ob + y, lambda copy: copy.wait_send())

    @pl.loop(0, o + 1)
    def _(ob):
        @pl.when(has_up)
        def _():
            for part in range(2):
                kv_copy(2 * ob + y, part, kv_up_sem, up).wait_send()
            kv_copy(2 * ob + 1 - y, 1, kv_up_sem, up).wait_send()

        @pl.when((ob < o) | (y == 0))
        def _():
            kv_copy(2 * ob + y, 0, kv_side_sem, side).wait_send()

        @pl.when((ob < o) | (y == 1))
        def _():
            side_copy(ob, 0).wait_send()

        @pl.when(ob < o)
        def _():
            for part in range(2):
                down_copy(ob, part).wait_send()
            cross_copy(ob).wait_send()

    @pl.when((y == 0) | has_up)
    def _():
        kv_copy(me, 1, kv_side_sem, side).wait_send()

    @pl.when((y == 1) | has_up)
    def _():
        side_copy(o, 1).wait_send()


def write_kernel(*refs):
    for src, dst in zip(refs[:4], refs[4:]):
        dst[...] = src[...]


def on_device(n, tp_count, hidden, key_weight, queries, values, map_out, log_sums, out_grad, mixing, out_gain):
    rows = queries.shape[0]
    heads = mixing.shape[0]
    width = values.shape[1]
    groups = width // V_DIM
    outer = n // 2
    vm = pl.BlockSpec(memory_space=VMEM)
    hops = pltpu.SemaphoreType.DMA((outer, 2))
    results = pl.pallas_call(
        functools.partial(attend_kernel, n, tp_count, heads, groups),
        out_shape=(
            jax.ShapeDtypeStruct(queries.shape, jnp.bfloat16),
            jax.ShapeDtypeStruct((rows, width), jnp.bfloat16),
            jax.ShapeDtypeStruct((rows, width), jnp.bfloat16),
            jax.ShapeDtypeStruct((hidden.shape[1] // n, width), jnp.float32),
        ),
        in_specs=[vm] * 8 + [pl.BlockSpec(memory_space=pltpu.SMEM)],
        out_specs=(vm, vm, vm, vm),
        scratch_shapes=[
            VMEM((rows, heads * V_DIM), jnp.bfloat16),
            VMEM((2 * heads, rows), jnp.float32),
            VMEM((2 * heads * HEAD_DIM, rows), jnp.float32),
            VMEM((n, 2, rows, width), jnp.bfloat16),
            VMEM((outer, 2, rows, width), jnp.float32),
        ]
        + [VMEM((outer, 2, rows, width), jnp.bfloat16)] * 4
        + [
            VMEM((outer, rows, width), jnp.bfloat16),
            VMEM((tp_count, n, rows // tp_count, hidden.shape[1] // n), jnp.bfloat16),
            VMEM((n, rows, width), jnp.bfloat16),
        ]
        + [pltpu.SemaphoreType.DMA((n, 2))] * 3
        + [hops] * 4
        + [pltpu.SemaphoreType.DMA((outer,))] * 2
        + [pltpu.SemaphoreType.DMA]
        + [pltpu.SemaphoreType.DMA((size,)) for size in (tp_count, tp_count, n, outer, outer, outer)],
        compiler_params=pltpu.CompilerParams(
            vmem_limit_bytes=60 * 2**20, collective_id=0, has_side_effects=True
        ),
        cost_estimate=pl.CostEstimate(flops=5 * 10**9, bytes_accessed=10**7, transcendentals=0),
    )(hidden, key_weight, values, queries, map_out, out_grad, log_sums, out_gain.reshape(1, V_DIM), mixing)
    return pl.pallas_call(
        write_kernel,
        out_shape=tuple(jax.ShapeDtypeStruct(r.shape, r.dtype) for r in results),
        in_specs=[vm] * 4,
        out_specs=(vm,) * 4,
        cost_estimate=pl.CostEstimate(flops=10**6, bytes_accessed=4 * 10**6, transcendentals=0),
    )(*results)


def solution(mesh):
    placed = (
        P("sp", None),
        P(None, "tp"),
        P("sp", "tp"),
        P("sp", "tp"),
        P("sp", "tp"),
        P("tp", "sp"),
        P("sp", "tp"),
        P("tp"),
        P(),
    )
    return jax.shard_map(
        functools.partial(on_device, mesh.shape["sp"], mesh.shape["tp"]),
        mesh=mesh,
        in_specs=placed,
        out_specs=(P("sp", "tp"), P("sp", "tp"), P("sp", "tp"), P("sp", "tp")),
        check_vma=False,
    )
```
